32 devices in a mesh: kv: 16 (over z, y, x), tp: 2 (over core).
Axes of the slice: x: 2, y: 2, z: 4, core: 2. Of those that a mesh axis runs over, the one named last changes fastest.
Arguments:
- tokens: bfloat16 [256, 2048], P('kv', 'tp'), may hold values from -20 to 20
- attn_gain: bfloat16 [2048], replicated, may hold values from 0.099609375 to 1.8984375
- query_weight: bfloat16 [2048, 1024], P(None, 'tp'), may hold values from -0.125 to 0.125
- key_weight: bfloat16 [2048, 1024], P(None, 'tp'), may hold values from -0.125 to 0.125
- value_weight: bfloat16 [2048, 1024], P(None, 'tp'), may hold values from -0.125 to 0.125
- outgate_weight: bfloat16 [2048, 1024], P(None, 'tp'), may hold values from -0.125 to 0.125
- gate_weight: bfloat16 [2, 8, 2048], replicated, may hold values from -0.125 to 0.125
- forget_bias: float32 [8], replicated, may hold values from -1 to 4
- state_matrix: float32 [256, 8, 128, 128], P('kv', 'tp'), may hold values from -1.8 to 1.8
- state_norm: float32 [256, 8, 128], P('kv', 'tp'), may hold values from -1.8 to 1.8
- state_max: float32 [256, 8], P('kv', 'tp'), may hold values from -1 to 1
- out_weight: bfloat16 [1024, 2048], P(None, 'tp'), may hold values from -0.1875 to 0.1875
- mlp_gain: bfloat16 [2048], P('tp'), may hold values from 0.099609375 to 1.8984375
- up_weight: bfloat16 [2048, 8192], P('tp', 'kv'), may hold values from -0.125 to 0.125
- down_weight: bfloat16 [8192, 2048], P('kv', 'tp'), may hold values from -0.0625 to 0.0625
Outputs:
- result: bfloat16 [256, 2048], P('kv', 'tp')
- next_matrix: float32 [256, 8, 128, 128], P('kv', 'tp')
- next_norm: float32 [256, 8, 128], P('kv', 'tp')
- next_max: float32 [256, 8], P('kv', 'tp')
The draws below stay inside these ranges and needn't reach their ends.
All inputs are finite; a program needn't handle non-finite values.
Results may differ from the reference program's by a relative error of at most 0.013.
Values may be sent and summed in bfloat16 or wider, within the bound.
A program may use at most 64 MiB of HBM per device.

```python
import jax
import jax.numpy as jnp
from jax import lax

D = 2048
HEADS = 8
HEAD_DIM = 128
FF = 8192
MIX = 1024
BATCH = 256


def draw_tokens(key, part):
    column_scale = 1.0 + 3.0 * jnp.arange(D, dtype=jnp.float32) / D
    entries = jnp.clip(jax.random.normal(jax.random.fold_in(key, 13), (BATCH, D), jnp.float32), -5.0, 5.0)
    return (entries * column_scale).astype(jnp.bfloat16)


def block_scale(own_key, dims, pieces, least, largest):
    def one(dim, parts):
        steps = jax.random.uniform(jax.random.fold_in(jax.random.fold_in(own_key, 6), dim), (parts,), jnp.float32, least / len(pieces), largest / len(pieces))
        return jnp.repeat(jnp.exp(steps), dims[dim] // parts).reshape((-1,) + (1,) * (len(dims) - dim - 1))

    gain = one(*pieces[0])
    for cut in pieces[1:]:
        gain = gain * one(*cut)
    return gain


def bell_draw(stream_key, dims, spread, most, cuts=(), kind=jnp.bfloat16):
    level = block_scale(stream_key, dims, cuts, -0.22, 0.18) if cuts else 1.0
    drawn = jax.random.normal(stream_key, dims, jnp.float32) * spread * level
    return jnp.minimum(jnp.maximum(drawn, -most), most).astype(kind)


def setup_inputs(seed: int = 0) -> dict:
    arg_keys = jax.random.split(jax.random.key(seed), 16)
    tokens = draw_tokens(jax.random.fold_in(arg_keys[15], 71), 0)
    attn_gain = jnp.clip(1.0 + 0.18 * jax.random.normal(arg_keys[1], (D,), jnp.float32), 0.099609375, 1.8984375).astype(jnp.bfloat16)
    query_weight = bell_draw(arg_keys[2], (D, MIX), D ** -0.5, 0.125, ((1, 2),))
    key_weight = bell_draw(arg_keys[3], (D, MIX), D ** -0.5, 0.125, ((1, 2),))
    value_weight = bell_draw(arg_keys[4], (D, MIX), D ** -0.5, 0.125, ((1, 2),))
    outgate_weight = bell_draw(arg_keys[5], (D, MIX), D ** -0.5, 0.125, ((1, 2),))
    gate_weight = bell_draw(arg_keys[6], (2, HEADS, D), D ** -0.5, 0.125)
    forget_bias = jnp.clip(jax.random.uniform(arg_keys[7], (HEADS,), jnp.float32, -1.0, 4.0), -1.0, 4.0)
    state_matrix = bell_draw(arg_keys[8], (BATCH, HEADS, HEAD_DIM, HEAD_DIM), 0.3, 1.8, ((0, 16), (1, 2)), jnp.float32)
    state_norm = bell_draw(arg_keys[9], (BATCH, HEADS, HEAD_DIM), 0.3, 1.8, ((0, 16), (1, 2)), jnp.float32)
    state_max = jnp.clip(jax.random.uniform(arg_keys[10], (BATCH, HEADS), jnp.float32, -1.0, 1.0) * block_scale(arg_keys[10], (BATCH, HEADS), ((0, 16), (1, 2)), -0.4, 0.0), -1.0, 1.0)
    out_weight = bell_draw(arg_keys[11], (MIX, D), MIX ** -0.5, 0.1875, ((1, 2),))
    mlp_gain = jnp.clip(1.0 + 0.18 * jax.random.normal(arg_keys[12], (D,), jnp.float32), 0.099609375, 1.8984375).astype(jnp.bfloat16)
    up_weight = bell_draw(arg_keys[13], (D, FF), D ** -0.5, 0.125, ((0, 2), (1, 16)))
    down_weight = bell_draw(arg_keys[14], (FF, D), FF ** -0.5, 0.0625, ((0, 16), (1, 2)))
    return {"tokens": tokens, "attn_gain": attn_gain, "query_weight": query_weight, "key_weight": key_weight, "value_weight": value_weight, "outgate_weight": outgate_weight, "gate_weight": gate_weight, "forget_bias": forget_bias, "state_matrix": state_matrix, "state_norm": state_norm, "state_max": state_max, "out_weight": out_weight, "mlp_gain": mlp_gain, "up_weight": up_weight, "down_weight": down_weight}


epsilon = 1e-06

def reference(tokens, attn_gain, query_weight, key_weight, value_weight, outgate_weight, gate_weight, forget_bias, state_matrix, state_norm, state_max, out_weight, mlp_gain, up_weight, down_weight):
    values = tokens.astype(jnp.float32)
    batch = tokens.shape[0]
    model_width = values.shape[1]
    scale_in = lax.rsqrt(lax.optimization_barrier(jnp.sum(values * values, axis=1)) / model_width + epsilon)
    scaled_in = (values * attn_gain.astype(jnp.float32)).astype(jnp.bfloat16)

    def project(weight):
        return jnp.dot(scaled_in, weight, preferred_element_type=jnp.float32) * scale_in[:, None]
    query_rows = project(query_weight).reshape(batch, HEADS, HEAD_DIM)
    key_rows = (project(key_weight) * HEAD_DIM ** (-0.5)).reshape(batch, HEADS, HEAD_DIM)
    value_rows = project(value_weight).reshape(batch, HEADS, HEAD_DIM)
    outgate = project(outgate_weight).reshape(batch, HEADS, HEAD_DIM)
    gate_rows = gate_weight.reshape(2 * HEADS, model_width)
    gate_pre = jnp.einsum('sd,gd->sg', scaled_in, gate_rows, preferred_element_type=jnp.float32) * scale_in[:, None]
    in_gate = gate_pre[:, :HEADS]
    forget_log = jax.nn.log_sigmoid(gate_pre[:, HEADS:] + forget_bias)
    next_max = jnp.maximum(forget_log + state_max, in_gate)
    kept_share = jnp.exp(forget_log + state_max - next_max)
    admitted = jnp.exp(in_gate - next_max)
    next_matrix = kept_share[:, :, None, None] * state_matrix + admitted[:, :, None, None] * key_rows[:, :, :, None] * value_rows[:, :, None, :]
    next_norm = kept_share[:, :, None] * state_norm + admitted[:, :, None] * key_rows
    numerator = jnp.einsum('shd,shde->she', query_rows, next_matrix, precision=lax.Precision.HIGHEST)
    denominator = lax.optimization_barrier(jnp.sum(query_rows * next_norm, axis=2))
    head_out = numerator / jnp.maximum(jnp.abs(denominator), 1.0)[:, :, None]
    mixed = (head_out * jax.nn.sigmoid(outgate)).reshape(batch, HEADS * HEAD_DIM).astype(jnp.bfloat16)
    attended = jnp.dot(mixed, out_weight, preferred_element_type=jnp.float32)
    residual = (values + attended).astype(jnp.bfloat16)
    res_values = residual.astype(jnp.float32)
    scale_mid = lax.rsqrt(lax.optimization_barrier(jnp.sum(res_values * res_values, axis=1)) / model_width + epsilon)
    scaled_mid = (res_values * mlp_gain.astype(jnp.float32)).astype(jnp.bfloat16)
    up_value = jnp.dot(scaled_mid, up_weight, preferred_element_type=jnp.float32) * scale_mid[:, None]
    hidden = jnp.square(jax.nn.relu(up_value)).astype(jnp.bfloat16)
    result = (res_values + jnp.dot(hidden, down_weight, preferred_element_type=jnp.float32)).astype(jnp.bfloat16)
    return (result, next_matrix, next_norm, next_max)
```

```python
import functools

import jax
import jax.numpy as jnp
from jax import lax
from jax.experimental import pallas as pl
from jax.experimental.pallas import tpu as pltpu
from jax.sharding import PartitionSpec as P

epsilon = 1e-06
MESH = pl.DeviceIdType.MESH


def partner_of(index, step, count):
    if count & (count - 1):
        return lax.rem(index + step, count), lax.rem(index + count - step, count)
    out = 0
    bit = 1
    while bit < count:
        digit = lax.rem(lax.div(index, bit), 2)
        out = out + bit * (1 - digit if step & bit else digit)
        bit *= 2
    return out, out


def mixer_kernel(
    layers,
    plane,
    cores,
    model_width,
    tokens_ref,
    mixed_ref,
    gain_ref,
    out_hbm,
    up_hbm,
    down_hbm,
    result_ref,
    out_w,
    up_w,
    down_w,
    mixed_all,
    rows_all,
    up_own,
    part_send,
    part_all,
    down_own,
    near_send,
    near_all,
    far_send,
    far_all,
    load_sem,
    mixed_send_sem,
    mixed_recv_sem,
    row_send_sem,
    row_recv_sem,
    part_send_sem,
    part_recv_sem,
    near_send_sem,
    near_recv_sem,
    far_send_sem,
    far_recv_sem,
):
    rows = tokens_ref.shape[0]
    width = mixed_ref.shape[1]
    hidden_width = up_w.shape[1]
    me = lax.axis_index("kv")
    core = lax.axis_index("tp")
    layer = lax.div(me, plane)
    spot = lax.rem(me, plane)
    loads = [
        pltpu.make_async_copy(src, dst, load_sem.at[i])
        for i, (src, dst) in enumerate(((out_hbm, out_w), (up_hbm, up_w), (down_hbm, down_w)))
    ]
    for load in loads:
        load.start()
    layer_steps = [partner_of(layer, s, layers) for s in range(layers)]
    spot_steps = [partner_of(spot, s, plane) for s in range(plane)]
    core_steps = [partner_of(core, s, cores) for s in range(cores)]

    def kv_id(at_layer, at_spot):
        return {"kv": at_layer * plane + at_spot}

    barrier = pltpu.get_barrier_semaphore()
    for s in range(1, cores):
        pl.semaphore_signal(barrier, inc=1, device_id={"tp": core_steps[s][0]}, device_id_type=MESH)
    for s in range(1, plane):
        pl.semaphore_signal(
            barrier, inc=1, device_id=kv_id(layer, spot_steps[s][0]), device_id_type=MESH
        )
    for s in range(1, layers):
        pl.semaphore_signal(
            barrier, inc=1, device_id=kv_id(layer_steps[s][0], spot), device_id_type=MESH
        )
    pl.semaphore_wait(barrier, cores + plane + layers - 3)

    started = []

    def send(src, dst, send_sem, recv_sem, device):
        copy = pltpu.make_async_remote_copy(
            src_ref=src,
            dst_ref=dst,
            send_sem=send_sem,
            recv_sem=recv_sem,
            device_id=device,
            device_id_type=MESH,
        )
        copy.start()
        started.append(copy)

    def arrived(ref, sem):
        pltpu.make_async_copy(ref, ref, sem).wait()

    for s in range(1, cores):
        send(
            mixed_ref,
            mixed_all.at[s],
            mixed_send_sem.at[s],
            mixed_recv_sem.at[s],
            {"tp": core_steps[s][0]},
        )
    loads[0].wait()

    def out_part(values, owner):
        block = out_w[pl.ds(pl.multiple_of(owner * width, width), width), :]
        return jnp.dot(values, block, preferred_element_type=jnp.float32)

    attended = out_part(mixed_ref[...], core)
    for s in range(1, cores):
        arrived(mixed_all.at[s], mixed_recv_sem.at[s])
        attended = attended + out_part(mixed_all[s], core_steps[s][1])
    residual = (tokens_ref[...].astype(jnp.float32) + attended).astype(jnp.bfloat16)
    rows_all[0, 0] = residual
    for s in range(1, layers):
        send(
            rows_all.at[0, 0],
            rows_all.at[s, 0],
            row_send_sem.at[s, 0],
            row_recv_sem.at[s, 0],
            kv_id(layer_steps[s][0], spot),
        )

    def spread(g):
        for s in range(1, plane):
            send(
                rows_all.at[g, 0],
                rows_all.at[g, s],
                row_send_sem.at[g, s],
                row_recv_sem.at[g, s],
                kv_id(layer, spot_steps[s][0]),
            )

    spread(0)
    gain = gain_ref[...].astype(jnp.float32)
    group = plane * rows

    def up_stage(g):
        if g + 1 < layers:
            arrived(rows_all.at[g + 1, 0], row_recv_sem.at[g + 1, 0])
            spread(g + 1)
        for s in range(1, plane):
            arrived(rows_all.at[g, s], row_recv_sem.at[g, s])
        if g == 0:
            loads[1].wait()
        values = rows_all[g].reshape(group, -1).astype(jnp.float32)
        squares = jnp.sum(values * values, axis=1, keepdims=True)
        high = squares.astype(jnp.bfloat16).astype(jnp.float32)
        lanes = lax.broadcasted_iota(jnp.int32, (group, 128), 1)
        part_send[g, :, hidden_width:] = jnp.where(lanes < 64, high, squares - high).astype(jnp.bfloat16)
        scaled = (values * gain).astype(jnp.bfloat16)
        partial = jnp.dot(scaled, up_w[...], preferred_element_type=jnp.float32)
        part_send[g, :, :hidden_width] = partial.astype(jnp.bfloat16)
        for s in range(1, cores):
            send(
                part_send.at[g],
                part_all.at[g, s],
                part_send_sem.at[g, s],
                part_recv_sem.at[g, s],
                {"tp": core_steps[s][0]},
            )
        up_own[g, :, :hidden_width] = partial
        up_own[g, :, hidden_width:] = jnp.broadcast_to(squares, (group, 128))

    def down_stage(g):
        total = up_own[g, :, :hidden_width]
        squares = up_own[g, :, hidden_width : hidden_width + 1]
        for s in range(1, cores):
            arrived(part_all.at[g, s], part_recv_sem.at[g, s])
            total = total + part_all[g, s, :, :hidden_width].astype(jnp.float32)
            tail = part_all[g, s, :, hidden_width:].astype(jnp.float32)
            squares = squares + tail[:, 0:1] + tail[:, 64:65]
        up_value = total * lax.rsqrt(squares / model_width + epsilon)
        hidden = jnp.square(jnp.maximum(up_value, 0.0)).astype(jnp.bfloat16)
        if g == 0:
            loads[2].wait()
        share = jnp.dot(hidden, down_w[...], preferred_element_type=jnp.float32)
        down_own[g] = share[:rows]
        near_send[g] = share.astype(jnp.bfloat16).reshape(near_send.shape[1:])
        for s in range(1, plane):
            send(
                near_send.at[g, s],
                near_all.at[g, s],
                near_send_sem.at[g, s],
                near_recv_sem.at[g, s],
                kv_id(layer, spot_steps[s][1]),
            )

    def plane_sum(g):
        total = down_own[g]
        for s in range(1, plane):
            arrived(near_all.at[g, s], near_recv_sem.at[g, s])
            total = total + near_all[g, s].astype(jnp.float32)
        return total

    def far_stage(g):
        total = plane_sum(g)
        if g == 0:
            down_own[0] = total
            return
        far_send[g] = total.astype(jnp.bfloat16)
        send(
            far_send.at[g],
            far_all.at[g],
            far_send_sem.at[g],
            far_recv_sem.at[g],
            kv_id(layer_steps[g][1], spot),
        )

    for g in range(layers + 2):
        if g < layers:
            up_stage(g)
        if 0 <= g - 1 < layers:
            down_stage(g - 1)
        if 0 <= g - 2 < layers:
            far_stage(g - 2)
    total = down_own[0]
    for s in range(1, layers):
        arrived(far_all.at[s], far_recv_sem.at[s])
        total = total + far_all[s].astype(jnp.float32)
    result_ref[...] = (rows_all[0, 0].astype(jnp.float32) + total).astype(jnp.bfloat16)
    for copy in started:
        copy.wait_send()


def channel_mixer(tokens, mixed, mlp_gain, out_weight, up_weight, down_weight, model_width):
    count = lax.axis_size("kv")
    cores = lax.axis_size("tp")
    plane = 4 if count % 4 == 0 else 1
    layers = count // plane
    rows, features = tokens.shape
    hidden_width = up_weight.shape[1]
    group = plane * rows
    bf16, f32, dma = jnp.bfloat16, jnp.float32, pltpu.SemaphoreType.DMA
    vmem = pl.BlockSpec(memory_space=pltpu.VMEM)
    anywhere = pl.BlockSpec(memory_space=pl.ANY)
    return pl.pallas_call(
        functools.partial(mixer_kernel, layers, plane, cores, model_width),
        out_shape=jax.ShapeDtypeStruct((rows, features), bf16),
        in_specs=[vmem] * 3 + [anywhere] * 3,
        out_specs=vmem,
        scratch_shapes=[
            pltpu.VMEM(out_weight.shape, bf16),
            pltpu.VMEM(up_weight.shape, bf16),
            pltpu.VMEM(down_weight.shape, bf16),
            pltpu.VMEM((cores,) + mixed.shape, bf16),
            pltpu.VMEM((layers, plane, rows, features), bf16),
            pltpu.VMEM((layers, group, hidden_width + 128), f32),
            pltpu.VMEM((layers, group, hidden_width + 128), bf16),
            pltpu.VMEM((layers, cores, group, hidden_width + 128), bf16),
            pltpu.VMEM((layers, rows, features), f32),
            pltpu.VMEM((layers, plane, rows, features), bf16),
            pltpu.VMEM((layers, plane, rows, features), bf16),
            pltpu.VMEM((layers, rows, features), bf16),
            pltpu.VMEM((layers, rows, features), bf16),
            dma((3,)),
            dma((cores,)),
            dma((cores,)),
            dma((layers, plane)),
            dma((layers, plane)),
            dma((layers, cores)),
            dma((layers, cores)),
            dma((layers, plane)),
            dma((layers, plane)),
            dma((layers,)),
            dma((layers,)),
        ],
        compiler_params=pltpu.CompilerParams(collective_id=0, has_side_effects=True),
        name="channel_mixer",
    )(tokens, mixed, mlp_gain.reshape(1, features), out_weight, up_weight, down_weight)


def body(
    tokens,
    attn_gain,
    query_weight,
    key_weight,
    value_weight,
    outgate_weight,
    gate_weight,
    forget_bias,
    state_matrix,
    state_norm,
    state_max,
    out_weight,
    mlp_gain,
    up_weight,
    down_weight,
):
    sequences = tokens.shape[0]
    local_heads = state_matrix.shape[1]
    head_dim = state_matrix.shape[2]
    width = query_weight.shape[1]
    model_width = attn_gain.shape[0]
    first_head = lax.axis_index("tp") * local_heads
    my_gates = lax.dynamic_slice_in_dim(gate_weight, first_head, local_heads, 1).reshape(
        2 * local_heads, model_width
    )
    my_bias = lax.dynamic_slice_in_dim(forget_bias, first_head, local_heads, 0)
    gain_full = attn_gain.astype(jnp.float32)
    seg_values = lax.all_gather(tokens, "tp", axis=1, tiled=True).astype(jnp.float32)
    scaled = (seg_values * gain_full).astype(jnp.bfloat16)

    def product(weight):
        return jnp.dot(scaled, weight, preferred_element_type=jnp.float32)

    gate_part = jnp.einsum("sd,gd->sg", scaled, my_gates, preferred_element_type=jnp.float32)
    squares = jnp.sum(seg_values * seg_values, axis=1)
    query_acc = product(query_weight)
    key_acc = product(key_weight)
    value_acc = product(value_weight)
    outgate_acc = product(outgate_weight)
    scale_in = lax.rsqrt(squares / model_width + epsilon)[:, None]
    query_rows = (query_acc * scale_in).reshape(sequences, local_heads, head_dim)
    key_rows = (key_acc * scale_in * head_dim ** (-0.5)).reshape(sequences, local_heads, head_dim)
    value_rows = (value_acc * scale_in).reshape(sequences, local_heads, head_dim)
    outgate = (outgate_acc * scale_in).reshape(sequences, local_heads, head_dim)
    gate_pre = gate_part * scale_in
    in_gate = gate_pre[:, :local_heads]
    forget_log = jax.nn.log_sigmoid(gate_pre[:, local_heads:] + my_bias)
    next_max = jnp.maximum(forget_log + state_max, in_gate)
    kept_share = jnp.exp(forget_log + state_max - next_max)
    admitted = jnp.exp(in_gate - next_max)
    next_matrix = (
        kept_share[:, :, None, None] * state_matrix
        + admitted[:, :, None, None] * key_rows[:, :, :, None] * value_rows[:, :, None, :]
    )
    next_norm = kept_share[:, :, None] * state_norm + admitted[:, :, None] * key_rows
    numerator = jnp.einsum(
        "shd,shde->she", query_rows, next_matrix, precision=lax.Precision.HIGHEST
    )
    denominator = jnp.sum(query_rows * next_norm, axis=2)
    head_out = numerator / jnp.maximum(jnp.abs(denominator), 1.0)[:, :, None]
    mixed = (head_out * jax.nn.sigmoid(outgate)).reshape(sequences, width).astype(jnp.bfloat16)
    result = channel_mixer(
        tokens, mixed, mlp_gain, out_weight, up_weight, down_weight, model_width
    )
    return (result, next_matrix, next_norm, next_max)


def solution(mesh):
    in_specs = (
        P("kv", "tp"),
        P(),
        P(None, "tp"),
        P(None, "tp"),
        P(None, "tp"),
        P(None, "tp"),
        P(),
        P(),
        P("kv", "tp", None, None),
        P("kv", "tp", None),
        P("kv", "tp"),
        P(None, "tp"),
        P("tp"),
        P("tp", "kv"),
        P("kv", "tp"),
    )
    out_specs = (P("kv", "tp"), P("kv", "tp", None, None), P("kv", "tp", None), P("kv", "tp"))
    return jax.shard_map(body, mesh=mesh, in_specs=in_specs, out_specs=out_specs, check_vma=False)
```

```python
import functools

import jax
import jax.numpy as jnp
from jax import lax
from jax.experimental import pallas as pl
from jax.experimental.pallas import tpu as pltpu
from jax.sharding import PartitionSpec as P

epsilon = 1e-06
MESH = pl.DeviceIdType.MESH


def partner_of(index, step, count):
    if count & (count - 1):
        return lax.rem(index + step, count), lax.rem(index + count - step, count)
    out = 0
    bit = 1
    while bit < count:
        digit = lax.rem(lax.div(index, bit), 2)
        out = out + bit * (1 - digit if step & bit else digit)
        bit *= 2
    return out, out


def mixer_kernel(
    layers,
    plane,
    cores,
    model_width,
    tokens_ref,
    attn_gain_ref,
    gate_ref,
    bias_ref,
    norm_ref,
    max_ref,
    gain_ref,
    query_hbm,
    key_hbm,
    value_hbm,
    outgate_hbm,
    state_hbm,
    out_hbm,
    up_hbm,
    down_hbm,
    result_ref,
    matrix_hbm,
    next_norm_ref,
    next_max_ref,
    column_ref,
    value_ref,
    kept_ref,
    query_w,
    key_w,
    value_w,
    outgate_w,
    state,
    tokens_all,
    query_t,
    numer,
    mixed_ref,
    token_send_sem,
    token_recv_sem,
    store_sem,
    out_w,
    up_w,
    down_w,
    mixed_all,
    rows_all,
    up_own,
    part_send,
    part_all,
    down_own,
    near_send,
    near_all,
    far_send,
    far_all,
    load_sem,
    mixed_send_sem,
    mixed_recv_sem,
    row_send_sem,
    row_recv_sem,
    part_send_sem,
    part_recv_sem,
    near_send_sem,
    near_recv_sem,
    far_send_sem,
    far_recv_sem,
):
    rows, features = tokens_ref.shape
    heads, head_dim = norm_ref.shape[1:]
    width = mixed_ref.shape[1]
    hidden_width = up_w.shape[1]
    me = lax.axis_index("kv")
    core = lax.axis_index("tp")
    layer = lax.div(me, plane)
    spot = lax.rem(me, plane)
    loads = [
        pltpu.make_async_copy(src, dst, load_sem.at[i])
        for i, (src, dst) in enumerate(
            (
                (key_hbm, key_w),
                (query_hbm, query_w),
                (value_hbm, value_w),
                (outgate_hbm, outgate_w),
                (state_hbm, state),
                (out_hbm, out_w),
                (up_hbm, up_w),
                (down_hbm, down_w),
            )
        )
    ]
    for load in loads:
        load.start()
    layer_steps = [partner_of(layer, s, layers) for s in range(layers)]
    spot_steps = [partner_of(spot, s, plane) for s in range(plane)]
    core_steps = [partner_of(core, s, cores) for s in range(cores)]

    def kv_id(at_layer, at_spot):
        return {"kv": at_layer * plane + at_spot}

    barrier = pltpu.get_barrier_semaphore()
    for s in range(1, cores):
        pl.semaphore_signal(barrier, inc=1, device_id={"tp": core_steps[s][0]}, device_id_type=MESH)
    for s in range(1, plane):
        pl.semaphore_signal(
            barrier, inc=1, device_id=kv_id(layer, spot_steps[s][0]), device_id_type=MESH
        )
    for s in range(1, layers):
        pl.semaphore_signal(
            barrier, inc=1, device_id=kv_id(layer_steps[s][0], spot), device_id_type=MESH
        )
    pl.semaphore_wait(barrier, cores + plane + layers - 3)

    started = []

    def send(src, dst, send_sem, recv_sem, device):
        copy = pltpu.make_async_remote_copy(
            src_ref=src,
            dst_ref=dst,
            send_sem=send_sem,
            recv_sem=recv_sem,
            device_id=device,
            device_id_type=MESH,
        )
        copy.start()
        started.append(copy)

    def arrived(ref, sem):
        pltpu.make_async_copy(ref, ref, sem).wait()

    for s in range(1, cores):
        send(
            tokens_ref,
            tokens_all.at[s],
            token_send_sem.at[s],
            token_recv_sem.at[s],
            {"tp": core_steps[s][0]},
        )
    parts = []
    squares_in = 0.0
    for s in range(cores):
        if s:
            arrived(tokens_all.at[s], token_recv_sem.at[s])
        block = (tokens_all[s] if s else tokens_ref[...]).astype(jnp.float32)
        owned = pl.ds(pl.multiple_of(core_steps[s][1] * features, features), features)
        squares_in = squares_in + jnp.sum(block * block, axis=1, keepdims=True)
        block_gain = attn_gain_ref[owned].astype(jnp.float32).reshape(1, features)
        parts.append((owned, (block * block_gain).astype(jnp.bfloat16)))
    scale_in = lax.rsqrt(squares_in / model_width + epsilon)
    gate_pre = sum(
        lax.dot_general(
            part, gate_ref[:, owned], (((1,), (1,)), ((), ())), preferred_element_type=jnp.float32
        )
        for owned, part in parts
    )
    gate_pre = gate_pre * scale_in
    all_heads = gate_pre.shape[1] // 2
    forget_pre = gate_pre[:, all_heads:] + bias_ref[...]
    forget_all = jnp.minimum(forget_pre, 0.0) - jnp.log1p(jnp.exp(-jnp.abs(forget_pre)))
    input_pre = gate_pre[:, :all_heads]
    gate_lane = lax.broadcasted_iota(jnp.int32, input_pre.shape, 1)
    diagonal = lax.broadcasted_iota(jnp.int32, (rows, rows), 0) == lax.broadcasted_iota(
        jnp.int32, (rows, rows), 1
    )
    kept, admitted = [], []
    for h in range(heads):
        mine = core * heads + h
        in_gate = jnp.sum(jnp.where(gate_lane == mine, input_pre, 0.0), axis=1, keepdims=True)
        forget_log = jnp.sum(jnp.where(gate_lane == mine, forget_all, 0.0), axis=1, keepdims=True)
        state_max = jnp.sum(jnp.where(diagonal, max_ref[h : h + 1, :], 0.0), axis=1, keepdims=True)
        level = forget_log + state_max
        next_max = jnp.maximum(level, in_gate)
        kept.append(jnp.exp(level - next_max))
        admitted.append(jnp.exp(in_gate - next_max))
        next_max_ref[h : h + 1, :] = jnp.sum(
            jnp.where(diagonal, next_max, 0.0), axis=0, keepdims=True
        )
        kept_ref[:, h : h + 1] = kept[h]

    def project(weight, load):
        load.wait()
        return sum(
            jnp.dot(part, weight[owned, :], preferred_element_type=jnp.float32)
            for owned, part in parts
        ) * scale_in

    def head(values, h):
        return values[:, h * head_dim : (h + 1) * head_dim]

    key_rows = project(key_w, loads[0]) * head_dim ** (-0.5)
    query_rows = project(query_w, loads[1])
    query_t[...] = query_rows.T
    column_ref[...] = jnp.concatenate(
        [admitted[h] * head(key_rows, h) for h in range(heads)], axis=1
    ).T
    value_rows = project(value_w, loads[2])
    value_ref[...] = value_rows
    outgate = jax.nn.sigmoid(project(outgate_w, loads[3]))
    loads[4].wait()
    for h in range(heads):
        for b in range(rows):
            column = query_t[h * head_dim : (h + 1) * head_dim, b : b + 1]
            numer[h, b : b + 1, :] = jnp.sum(column * state[b, h], axis=0, keepdims=True)
    for h in range(heads):
        query_head, key_head = head(query_rows, h), admitted[h] * head(key_rows, h)
        next_norm = kept[h] * norm_ref[:, h, :] + key_head
        next_norm_ref[:, h, :] = next_norm
        denominator = jnp.sum(query_head * next_norm, axis=1, keepdims=True)
        overlap = jnp.sum(query_head * key_head, axis=1, keepdims=True)
        numerator = kept[h] * numer[h] + overlap * head(value_rows, h)
        head_out = numerator / jnp.maximum(jnp.abs(denominator), 1.0)
        mixed_ref[:, h * head_dim : (h + 1) * head_dim] = (head_out * head(outgate, h)).astype(
            jnp.bfloat16
        )

    for s in range(1, cores):
        send(
            mixed_ref,
            mixed_all.at[s],
            mixed_send_sem.at[s],
            mixed_recv_sem.at[s],
            {"tp": core_steps[s][0]},
        )
    loads[5].wait()

    def out_part(values, owner):
        block = out_w[pl.ds(pl.multiple_of(owner * width, width), width), :]
        return jnp.dot(values, block, preferred_element_type=jnp.float32)

    attended = out_part(mixed_ref[...], core)
    for s in range(1, cores):
        arrived(mixed_all.at[s], mixed_recv_sem.at[s])
        attended = attended + out_part(mixed_all[s], core_steps[s][1])
    residual = (tokens_ref[...].astype(jnp.float32) + attended).astype(jnp.bfloat16)
    rows_all[0, 0] = residual
    for s in range(1, layers):
        send(
            rows_all.at[0, 0],
            rows_all.at[s, 0],
            row_send_sem.at[s, 0],
            row_recv_sem.at[s, 0],
            kv_id(layer_steps[s][0], spot),
        )

    def spread(g):
        for s in range(1, plane):
            send(
                rows_all.at[g, 0],
                rows_all.at[g, s],
                row_send_sem.at[g, s],
                row_recv_sem.at[g, s],
                kv_id(layer, spot_steps[s][0]),
            )

    spread(0)
    stores = [
        pltpu.make_async_copy(state.at[b], matrix_hbm.at[b], store_sem.at[b]) for b in range(rows)
    ]

    def update(b):
        for h in range(heads):
            lanes = slice(h * head_dim, (h + 1) * head_dim)
            share = jnp.broadcast_to(kept_ref[b : b + 1, h : h + 1], (1, head_dim))
            state[b, h] = share * state[b, h] + column_ref[lanes, b : b + 1] * value_ref[
                b : b + 1, lanes
            ]

    gain = gain_ref[...].astype(jnp.float32).reshape(1, features)
    group = plane * rows

    def relay_stage(g):
        arrived(rows_all.at[g, 0], row_recv_sem.at[g, 0])
        spread(g)

    def up_stage(g):
        for b in range(g * rows // layers, (g + 1) * rows // layers):
            update(b)
            stores[b].start()
        for s in range(1, plane):
            arrived(rows_all.at[g, s], row_recv_sem.at[g, s])
        if g == 0:
            loads[6].wait()
        values = rows_all[g].reshape(group, -1).astype(jnp.float32)
        squares = jnp.sum(values * values, axis=1, keepdims=True)
        high = squares.astype(jnp.bfloat16).astype(jnp.float32)
        lanes = lax.broadcasted_iota(jnp.int32, (group, 128), 1)
        part_send[g, :, hidden_width:] = jnp.where(lanes < 64, high, squares - high).astype(jnp.bfloat16)
        scaled = (values * gain).astype(jnp.bfloat16)
        partial = jnp.dot(scaled, up_w[...], preferred_element_type=jnp.float32)
        part_send[g, :, :hidden_width] = partial.astype(jnp.bfloat16)
        for s in range(1, cores):
            send(
                part_send.at[g],
                part_all.at[g, s],
                part_send_sem.at[g, s],
                part_recv_sem.at[g, s],
                {"tp": core_steps[s][0]},
            )
        up_own[g, :, :hidden_width] = partial
        up_own[g, :, hidden_width:] = jnp.broadcast_to(squares, (group, 128))

    def down_stage(g):
        total = up_own[g, :, :hidden_width]
        squares = up_own[g, :, hidden_width : hidden_width + 1]
        for s in range(1, cores):
            arrived(part_all.at[g, s], part_recv_sem.at[g, s])
            total = total + part_all[g, s, :, :hidden_width].astype(jnp.float32)
            tail = part_all[g, s, :, hidden_width:].astype(jnp.float32)
            squares = squares + tail[:, 0:1] + tail[:, 64:65]
        up_value = total * lax.rsqrt(squares / model_width + epsilon)
        hidden = jnp.square(jnp.maximum(up_value, 0.0)).astype(jnp.bfloat16)
        if g == 0:
            loads[7].wait()
        share = jnp.dot(hidden, down_w[...], preferred_element_type=jnp.float32)
        down_own[g] = share[:rows]
        near_send[g] = share.astype(jnp.bfloat16).reshape(near_send.shape[1:])
        for s in range(1, plane):
            send(
                near_send.at[g, s],
                near_all.at[g, s],
                near_send_sem.at[g, s],
                near_recv_sem.at[g, s],
                kv_id(layer, spot_steps[s][1]),
            )

    def plane_sum(g):
        total = down_own[g]
        for s in range(1, plane):
            arrived(near_all.at[g, s], near_recv_sem.at[g, s])
            total = total + near_all[g, s].astype(jnp.float32)
        return total

    def far_stage(g):
        total = plane_sum(g)
        if g == 0:
            down_own[0] = total
            return
        far_send[g] = total.astype(jnp.bfloat16)
        send(
            far_send.at[g],
            far_all.at[g],
            far_send_sem.at[g],
            far_recv_sem.at[g],
            kv_id(layer_steps[g][1], spot),
        )

    for g in range(layers + 2):
        if g + 1 < layers:
            relay_stage(g + 1)
        if 0 <= g - 1 < layers:
            down_stage(g - 1)
        if g < layers:
            up_stage(g)
        if 0 <= g - 2 < layers:
            far_stage(g - 2)
    total = down_own[0]
    for s in range(1, layers):
        arrived(far_all.at[s], far_recv_sem.at[s])
        total = total + far_all[s].astype(jnp.float32)
    result_ref[...] = (rows_all[0, 0].astype(jnp.float32) + total).astype(jnp.bfloat16)
    for copy in started:
        copy.wait_send()
    for store in stores:
        store.wait()


def emit_kernel(*refs):
    sources, targets, held, (load_sem, store_sem) = refs[:4], refs[4:8], refs[8:12], refs[12:]
    pieces = []
    for source, target, via in zip(sources, targets, held):
        if len(source.shape) == 4:
            pieces += [(source.at[b], target.at[b], via.at[b]) for b in range(source.shape[0])]
        else:
            pieces.append((source, target, via))
    loads = [
        pltpu.make_async_copy(source, via, load_sem.at[i])
        for i, (source, _, via) in enumerate(pieces)
    ]
    stores = [
        pltpu.make_async_copy(via, target, store_sem.at[i])
        for i, (_, target, via) in enumerate(pieces)
    ]
    for load in loads:
        load.start()
    for load, store in zip(loads, stores):
        load.wait()
        store.start()
    for store in stores:
        store.wait()


def body(
    tokens,
    attn_gain,
    query_weight,
    key_weight,
    value_weight,
    outgate_weight,
    gate_weight,
    forget_bias,
    state_matrix,
    state_norm,
    state_max,
    out_weight,
    mlp_gain,
    up_weight,
    down_weight,
):
    count = lax.axis_size("kv")
    cores = lax.axis_size("tp")
    plane = 4 if count % 4 == 0 else 1
    layers = count // plane
    rows, features = tokens.shape
    heads, head_dim = state_norm.shape[1:]
    width = query_weight.shape[1]
    model_width = attn_gain.shape[0]
    all_heads = forget_bias.shape[0]
    hidden_width = up_weight.shape[1]
    group = plane * rows
    bf16, f32, dma = jnp.bfloat16, jnp.float32, pltpu.SemaphoreType.DMA
    vmem = pl.BlockSpec(memory_space=pltpu.VMEM)
    anywhere = pl.BlockSpec(memory_space=pl.ANY)
    shape = jax.ShapeDtypeStruct
    outputs = pl.pallas_call(
        functools.partial(mixer_kernel, layers, plane, cores, model_width),
        out_shape=(
            shape((rows, features), bf16),
            shape(state_matrix.shape, f32),
            shape(state_norm.shape, f32),
            shape((heads, rows), f32),
        ),
        in_specs=[vmem] * 7 + [anywhere] * 8,
        out_specs=(vmem, anywhere, vmem, vmem),
        scratch_shapes=[
            pltpu.VMEM((width, rows), f32),
            pltpu.VMEM((rows, width), f32),
            pltpu.VMEM((rows, heads), f32),
            pltpu.VMEM(query_weight.shape, bf16),
            pltpu.VMEM(key_weight.shape, bf16),
            pltpu.VMEM(value_weight.shape, bf16),
            pltpu.VMEM(outgate_weight.shape, bf16),
            pltpu.VMEM(state_matrix.shape, f32),
            pltpu.VMEM((cores,) + tokens.shape, bf16),
            pltpu.VMEM((width, rows), f32),
            pltpu.VMEM((heads, rows, head_dim), f32),
            pltpu.VMEM((rows, width), bf16),
            dma((cores,)),
            dma((cores,)),
            dma((rows,)),
            pltpu.VMEM(out_weight.shape, bf16),
            pltpu.VMEM(up_weight.shape, bf16),
            pltpu.VMEM(down_weight.shape, bf16),
            pltpu.VMEM((cores, rows, width), bf16),
            pltpu.VMEM((layers, plane, rows, features), bf16),
            pltpu.VMEM((layers, group, hidden_width + 128), f32),
            pltpu.VMEM((layers, group, hidden_width + 128), bf16),
            pltpu.VMEM((layers, cores, group, hidden_width + 128), bf16),
            pltpu.VMEM((layers, rows, features), f32),
            pltpu.VMEM((layers, plane, rows, features), bf16),
            pltpu.VMEM((layers, plane, rows, features), bf16),
            pltpu.VMEM((layers, rows, features), bf16),
            pltpu.VMEM((layers, rows, features), bf16),
            dma((8,)),
            dma((cores,)),
            dma((cores,)),
            dma((layers, plane)),
            dma((layers, plane)),
            dma((layers, cores)),
            dma((layers, cores)),
            dma((layers, plane)),
            dma((layers, plane)),
            dma((layers,)),
            dma((layers,)),
        ],
        compiler_params=pltpu.CompilerParams(
            collective_id=0, has_side_effects=True, vmem_limit_bytes=58000 * 1024
        ),
        name="layer",
    )(
        tokens,
        attn_gain,
        gate_weight.reshape(2 * all_heads, model_width),
        forget_bias.reshape(1, all_heads),
        state_norm,
        state_max.T,
        mlp_gain,
        query_weight,
        key_weight,
        value_weight,
        outgate_weight,
        state_matrix,
        out_weight,
        up_weight,
        down_weight,
    )
    result, next_matrix, next_norm, next_max = pl.pallas_call(
        emit_kernel,
        out_shape=tuple(shape(x.shape, x.dtype) for x in outputs),
        in_specs=[anywhere] * 4,
        out_specs=(anywhere,) * 4,
        scratch_shapes=[pltpu.VMEM(x.shape, x.dtype) for x in outputs]
        + [dma((rows + 3,)), dma((rows + 3,))],
        compiler_params=pltpu.CompilerParams(vmem_limit_bytes=58000 * 1024),
        name="emit",
    )(*outputs)
    return (result, next_matrix, next_norm, next_max.T)


def solution(mesh):
    in_specs = (
        P("kv", "tp"),
        P(),
        P(None, "tp"),
        P(None, "tp"),
        P(None, "tp"),
        P(None, "tp"),
        P(),
        P(),
        P("kv", "tp", None, None),
        P("kv", "tp", None),
        P("kv", "tp"),
        P(None, "tp"),
        P("tp"),
        P("tp", "kv"),
        P("kv", "tp"),
    )
    out_specs = (P("kv", "tp"), P("kv", "tp", None, None), P("kv", "tp", None), P("kv", "tp"))
    return jax.shard_map(body, mesh=mesh, in_specs=in_specs, out_specs=out_specs, check_vma=False)
```
